32 devices in a mesh: ep: 16 (over z, y, core), tp: 2 (over x).
Axes of the slice: x: 2, y: 2, z: 4, core: 2. Of those that a mesh axis runs over, the one named last changes fastest.
Arguments:
- tokens: bfloat16 [288, 1024], P('ep'), may hold values from -16 to 16
- delta_state: float32 [288, 4, 128, 128], P('ep', 'tp'), may hold values from -1.8 to 1.8
- mixer_gain: float32 [1024], replicated, may hold values from 0.1 to 1.9
- query_weight: bfloat16 [1024, 512], P(None, 'tp'), may hold values from -0.1875 to 0.1875
- key_weight: bfloat16 [1024, 512], P(None, 'tp'), may hold values from -0.1875 to 0.1875
- value_weight: bfloat16 [1024, 512], P(None, 'tp'), may hold values from -0.1875 to 0.1875
- write_weight: bfloat16 [1024, 4], P(None, 'tp'), may hold values from -0.1875 to 0.1875
- decay_weight: bfloat16 [1024, 4], P(None, 'tp'), may hold values from -0.1875 to 0.1875
- decay_rate: float32 [4], P('tp'), may hold values from 0.05 to 4
- decay_bias: float32 [4], P('tp'), may hold values from -2 to 1
- head_gain: float32 [128], replicated, may hold values from 0.1 to 1.9
- out_weight: bfloat16 [512, 1024], P('tp'), may hold values from -0.25 to 0.25
- channel_gain: float32 [1024], replicated, may hold values from 0.1 to 1.9
- routes: int32 [288, 6], P('ep'), may hold values from 0 to 15, all different within a row; in each aligned block of 18 rows (0 to 17, 18 to 35, ...) at most 13 rows name the same one
- route_weights: float32 [288, 6], P('ep'), may hold values from 0.1 to 1
- expert_gate: bfloat16 [16, 1024, 512], P('ep', None, 'tp'), may hold values from -0.1875 to 0.1875
- expert_up: bfloat16 [16, 1024, 512], P('ep', None, 'tp'), may hold values from -0.1875 to 0.1875
- expert_down: bfloat16 [16, 512, 1024], P('ep', 'tp'), may hold values from -0.25 to 0.25
- shared_gate: bfloat16 [1024, 512], P(None, 'tp'), may hold values from -0.1875 to 0.1875
- shared_up: bfloat16 [1024, 512], P(None, 'tp'), may hold values from -0.1875 to 0.1875
- shared_down: bfloat16 [512, 1024], P('tp'), may hold values from -0.25 to 0.25
Outputs:
- layer_out: bfloat16 [288, 1024], P('ep', 'tp')
- next_state: float32 [288, 4, 128, 128], P('ep', 'tp')
The draws below stay inside these ranges and needn't reach their ends.
Inputs may be any that keep to these rules, and one draw needn't show every extreme that they name: `routes`: each row names 6 different experts. In each aligned block of 18 rows (the rows of one ep index) no expert is named by more than 13 rows, a bound that some block reaches.
All inputs are finite; a program needn't handle non-finite values.
Results may differ from the reference program's by a relative error of at most 0.015.
Values may be sent and summed in bfloat16 or wider, within the bound.
A program may use at most 64 MiB of HBM per device.

```python
import math
import jax
import jax.numpy as jnp
import numpy as np
from jax import lax

D = 1024
HEADS = 4
HEAD_DIM = 128
D_EXPERT = 512
D_SHARED = 512
EXPERTS = 16
TOP_K = 6
SEQ_DEV = 18
CAP = 13
TOKENS = 288
N_EP = 16
N_TP = 2


def draw_tokens(key, part):
    entry_key, column_key = jax.random.split(jax.random.fold_in(key, 71))
    column_pos = jnp.arange(D, dtype=jnp.float32) / (D - 1)
    jitter = jnp.exp(jax.random.uniform(column_key, (D,), jnp.float32, jnp.log(0.7), jnp.log(1.4)))
    rise = jnp.exp(jnp.log(0.5) + column_pos * jnp.log(5.0))
    entries = jnp.clip(jax.random.normal(entry_key, (TOKENS, D), jnp.float32), -4.0, 4.0)
    return (entries * (rise * jitter)[None, :]).astype(jnp.bfloat16)


def levels(stream_key, extent, shards, low, top_value):
    loudness, own = 1.0, jax.random.fold_in(stream_key, 6)
    for position, shards_of in shards:
        heights = jnp.exp(jax.random.uniform(jax.random.fold_in(own, position), (shards_of,), jnp.float32, low / len(shards), top_value / len(shards)))
        loudness = loudness * jnp.repeat(heights, extent[position] // shards_of).reshape([-1 if axis == position else 1 for axis in range(len(extent))])
    return loudness


def deal_out(stream_key, own, number, rows, count, top, most, slope):
    ranking = jax.random.permutation(stream_key, count)
    heavy_load, common = shares(count, rows * top, most, slope, True), shares(count, rows * top, most, slope, False)
    places = jnp.arange(count)

    def named(tallies, rotation):
        used = int((tallies > 0).sum())
        fixed = max(1, used // 4)
        passed = fixed + (places - fixed + rotation * (used - fixed)) % max(1, count - fixed)
        return jnp.zeros((count,), jnp.int32).at[ranking[jnp.where(places < fixed, places, passed)]].set(jnp.asarray(tallies, jnp.int32))

    tallies = jnp.where(number % 4 == 0, named(heavy_load, number // 4), named(common, number - number // 4 - 1))
    mixed = jax.random.permutation(jax.random.fold_in(own, 3), count)
    source_of, sink = mixed[0:count // 2 * 2:2], mixed[1:count // 2 * 2:2]
    slack = jnp.minimum(tallies[source_of] - 1, most - tallies[sink]) // 2
    slack = jnp.where((source_of == ranking[0]) | (sink == ranking[0]) | (tallies[sink] == 0), 0, jnp.maximum(slack, 0))
    passed = jax.random.randint(jax.random.fold_in(own, 4), (count // 2,), 0, 1 << 20) % (slack + 1)
    tallies = tallies.at[source_of].add(-passed).at[sink].add(passed)
    members = jnp.searchsorted(jnp.cumsum(tallies), jnp.arange(rows * top), side="right").astype(jnp.int32)
    table = members.reshape(top, rows).T
    table = table[jax.random.permutation(jax.random.fold_in(own, 1), rows)]
    rotation = jax.random.randint(jax.random.fold_in(own, 2), (rows, 1), 0, top)
    return jnp.take_along_axis(table, (jnp.arange(top)[None, :] + rotation) % top, axis=1)


def shares(count, total, limit, skew, full):
    loads = [(1 << 20) // math.isqrt(rank ** skew) + 1 for rank in range(1, count + 1)]
    largest = limit if full else min(limit, max(-(-total // count), total * loads[0] // sum(loads)))
    least = 1 if total - largest >= count - 1 else 0
    counts, surplus = [largest] + [least] * (count - 1), total - largest - least * (count - 1)
    while surplus > 0:
        movable = [i for i in range(1, count) if counts[i] < largest] or [i for i in range(1, count) if counts[i] < limit]
        whole, budget = sum([loads[i] for i in movable]), surplus
        for i in movable:
            more = min(limit - counts[i], max(1, budget * loads[i] // whole), surplus)
            counts[i] = counts[i] + more
            surplus = surplus - more
    return np.array(counts)


def gaussian(own_key, shape, deviation, reach, shards=(), kind=jnp.bfloat16):
    drawn = jax.random.normal(own_key, shape, jnp.float32) * deviation
    if len(shards) > 0:
        drawn = levels(own_key, shape, shards, -0.22, 0.18) * drawn
    return jnp.clip(drawn, min=-reach, max=reach).astype(kind)


def setup_inputs(seed: int = 0) -> dict:
    seeds = jax.random.split(jax.random.key(seed), 22)
    tokens = draw_tokens(jax.random.fold_in(seeds[21], 71), 0)
    delta_state = gaussian(seeds[1], (TOKENS, HEADS, HEAD_DIM, HEAD_DIM), 0.3, 1.8, ((0, 16), (1, 2)), jnp.float32)
    mixer_gain = jnp.clip(1.0 + 0.18 * jax.random.normal(seeds[2], (D,), jnp.float32), 0.1, 1.9)
    query_weight = gaussian(seeds[3], (D, HEADS * HEAD_DIM), D ** -0.5, 0.1875, ((1, 2),))
    key_weight = gaussian(seeds[4], (D, HEADS * HEAD_DIM), D ** -0.5, 0.1875, ((1, 2),))
    value_weight = gaussian(seeds[5], (D, HEADS * HEAD_DIM), D ** -0.5, 0.1875, ((1, 2),))
    write_weight = gaussian(seeds[6], (D, HEADS), D ** -0.5, 0.1875, ((1, 2),))
    decay_weight = gaussian(seeds[7], (D, HEADS), D ** -0.5, 0.1875, ((1, 2),))
    decay_rate = jnp.clip(jnp.exp(math.log(4.0) - 4.3820266 * jax.random.uniform(seeds[8], (HEADS,), jnp.float32) ** levels(seeds[8], (HEADS,), ((0, 2),), -0.2, 0.2)), 0.05, 4.0)
    decay_bias = jnp.clip(-2.0 + 3.0 * jax.random.uniform(seeds[9], (HEADS,), jnp.float32) ** levels(seeds[9], (HEADS,), ((0, 2),), -0.2, 0.2), -2.0, 1.0)
    head_gain = jnp.clip(1.0 + 0.18 * jax.random.normal(seeds[10], (HEAD_DIM,), jnp.float32), 0.1, 1.9)
    out_weight = gaussian(seeds[11], (HEADS * HEAD_DIM, D), (HEADS * HEAD_DIM) ** -0.5, 0.25, ((0, 2),))
    channel_gain = jnp.clip(1.0 + 0.18 * jax.random.normal(seeds[12], (D,), jnp.float32), 0.1, 1.9)
    routes_keys = jax.random.split(jax.random.fold_in(seeds[13], 1), TOKENS // SEQ_DEV)
    routes_turns = jax.random.permutation(jax.random.fold_in(seeds[13], 3), TOKENS // SEQ_DEV)
    routes = jax.vmap(lambda own, number: deal_out(jax.random.fold_in(seeds[13], 2), own, number, SEQ_DEV, EXPERTS, TOP_K, CAP, 1))(routes_keys, routes_turns).reshape((TOKENS, TOP_K))
    route_weights = jnp.clip(jnp.exp(math.log(1.0) - 2.3025851 * jax.random.uniform(seeds[14], (TOKENS, TOP_K), jnp.float32) ** levels(seeds[14], (TOKENS, TOP_K), ((0, 16),), -0.2, 0.2)), 0.1, 1.0)
    expert_gate = gaussian(seeds[15], (EXPERTS, D, D_EXPERT), D ** -0.5, 0.1875, ((0, 16), (2, 2)))
    expert_up = gaussian(seeds[16], (EXPERTS, D, D_EXPERT), D ** -0.5, 0.1875, ((0, 16), (2, 2)))
    expert_down = gaussian(seeds[17], (EXPERTS, D_EXPERT, D), D_EXPERT ** -0.5, 0.25, ((0, 16), (1, 2)))
    shared_gate = gaussian(seeds[18], (D, D_SHARED), D ** -0.5, 0.1875, ((1, 2),))
    shared_up = gaussian(seeds[19], (D, D_SHARED), D ** -0.5, 0.1875, ((1, 2),))
    shared_down = gaussian(seeds[20], (D_SHARED, D), D_SHARED ** -0.5, 0.25, ((0, 2),))
    return dict(tokens=tokens, delta_state=delta_state, mixer_gain=mixer_gain, query_weight=query_weight, key_weight=key_weight, value_weight=value_weight, write_weight=write_weight, decay_weight=decay_weight, decay_rate=decay_rate, decay_bias=decay_bias, head_gain=head_gain, out_weight=out_weight, channel_gain=channel_gain, routes=routes, route_weights=route_weights, expert_gate=expert_gate, expert_up=expert_up, expert_down=expert_down, shared_gate=shared_gate, shared_up=shared_up, shared_down=shared_down)


EPS = 1e-06
ROUTED_SCALE = 2.5

def rms_rows(values, gain_vec):
    mean_square = lax.optimization_barrier(jnp.mean(values * values, axis=-1, keepdims=True))
    return values * lax.rsqrt(mean_square + EPS) * gain_vec.astype(jnp.float32)

def unit_heads(raw, heads, head_dim):
    shaped = raw.astype(jnp.float32).reshape(raw.shape[0], heads, head_dim)
    return shaped * lax.rsqrt(lax.optimization_barrier(jnp.sum(shaped * shaped, axis=-1, keepdims=True)) + EPS)

def group_sum(hidden, weight, groups):
    group_width = hidden.shape[1] // groups
    running = jnp.zeros((hidden.shape[0], weight.shape[1]), jnp.float32)
    for group_number in range(groups):
        lower = group_number * group_width
        product = jnp.dot(hidden[:, lower:lower + group_width], weight[lower:lower + group_width], preferred_element_type=jnp.float32)
        rounded = lax.optimization_barrier(product.astype(jnp.bfloat16))
        running = running + rounded.astype(jnp.float32)
    return running.astype(jnp.bfloat16)

def reference(tokens, delta_state, mixer_gain, query_weight, key_weight, value_weight, write_weight, decay_weight, decay_rate, decay_bias, head_gain, out_weight, channel_gain, routes, route_weights, expert_gate, expert_up, expert_down, shared_gate, shared_up, shared_down):
    rows_total = tokens.shape[0]
    normed = rms_rows(tokens.astype(jnp.float32), mixer_gain).astype(jnp.bfloat16)
    query_raw = jnp.dot(normed, query_weight, preferred_element_type=jnp.float32).astype(jnp.bfloat16)
    key_raw = jnp.dot(normed, key_weight, preferred_element_type=jnp.float32).astype(jnp.bfloat16)
    value_raw = jnp.dot(normed, value_weight, preferred_element_type=jnp.float32).astype(jnp.bfloat16)
    write_rate = jax.nn.sigmoid(jnp.dot(normed, write_weight, preferred_element_type=jnp.float32))
    decay_keep = jnp.exp(-decay_rate * jax.nn.softplus(jnp.dot(normed, decay_weight, preferred_element_type=jnp.float32) + decay_bias))
    query_unit = unit_heads(query_raw, HEADS, HEAD_DIM) * HEAD_DIM ** (-0.5)
    key_unit = unit_heads(key_raw, HEADS, HEAD_DIM)
    value_vec = value_raw.astype(jnp.float32).reshape(rows_total, HEADS, HEAD_DIM)
    held_state = decay_keep[:, :, None, None] * delta_state
    correction = value_vec - jnp.einsum('rhkv,rhk->rhv', held_state, key_unit, precision=lax.Precision.HIGHEST)
    next_state = held_state + write_rate[:, :, None, None] * key_unit[:, :, :, None] * correction[:, :, None, :]
    readout = jnp.einsum('rhkv,rhk->rhv', next_state, query_unit, precision=lax.Precision.HIGHEST)
    head_out = rms_rows(readout, head_gain).astype(jnp.bfloat16).reshape(rows_total, HEADS * HEAD_DIM)
    mixer_out = group_sum(head_out, out_weight, N_TP)
    residual = (tokens.astype(jnp.float32) + mixer_out.astype(jnp.float32)).astype(jnp.bfloat16)
    expert_input = rms_rows(residual.astype(jnp.float32), channel_gain).astype(jnp.bfloat16)
    weight_norm = route_weights / lax.optimization_barrier(jnp.sum(route_weights, axis=1, keepdims=True)) * ROUTED_SCALE
    pair_ids = routes.reshape(N_EP, SEQ_DEV * TOP_K)
    order_pos = jnp.arange(SEQ_DEV * TOP_K, dtype=jnp.int32)
    earlier = (pair_ids[:, :, None] == pair_ids[:, None, :]) & (order_pos[None, :, None] > order_pos[None, None, :])
    slot_index = lax.optimization_barrier(jnp.sum(earlier.astype(jnp.int32), axis=2))
    block_ids = jnp.arange(N_EP, dtype=jnp.int32)[:, None]
    expert_rows = N_EP * CAP
    slot_flat = (pair_ids * expert_rows + block_ids * CAP + slot_index).reshape(-1).astype(jnp.int32)
    token_ids = jnp.repeat(jnp.arange(rows_total, dtype=jnp.int32), TOP_K)
    row_token = jnp.full((EXPERTS * expert_rows,), rows_total, jnp.int32).at[slot_flat].set(token_ids)
    row_weight = jnp.zeros((EXPERTS * expert_rows,), jnp.float32).at[slot_flat].set(weight_norm.reshape(-1))
    padded_rows = jnp.concatenate([expert_input, jnp.zeros((1, D), jnp.bfloat16)], axis=0)

    def one_expert(inputs):
        gate_mat, up_mat, down_mat, token_list = inputs
        chosen = padded_rows[token_list]
        gate_val = jnp.dot(chosen, gate_mat, preferred_element_type=jnp.float32)
        up_val = jnp.dot(chosen, up_mat, preferred_element_type=jnp.float32)
        hidden_act = (jax.nn.silu(gate_val) * up_val).astype(jnp.bfloat16)
        return group_sum(hidden_act, down_mat, N_TP)
    expert_out = lax.map(one_expert, (expert_gate, expert_up, expert_down, row_token.reshape(EXPERTS, expert_rows)))
    weighted = row_weight[:, None] * expert_out.reshape(-1, D).astype(jnp.float32)
    routed = jnp.zeros((rows_total + 1, D), jnp.float32).at[row_token].add(weighted)[:rows_total]
    shared_act = (jax.nn.silu(jnp.dot(expert_input, shared_gate, preferred_element_type=jnp.float32)) * jnp.dot(expert_input, shared_up, preferred_element_type=jnp.float32)).astype(jnp.bfloat16)
    shared_out = group_sum(shared_act, shared_down, N_TP)
    layer_out = (residual.astype(jnp.float32) + routed + shared_out.astype(jnp.float32)).astype(jnp.bfloat16)
    return (layer_out, next_state)
```

```python
import functools

import jax
import jax.numpy as jnp
from jax import lax
from jax.experimental import pallas as pl
from jax.experimental.pallas import tpu as pltpu
from jax.sharding import PartitionSpec as P

EPS = 1e-06
ROUTED_SCALE = 2.5
MESH = pl.DeviceIdType.MESH
F32 = jnp.float32
BF16 = jnp.bfloat16


def rms_rows(values, gain_row):
    mean_square = jnp.mean(values * values, axis=-1, keepdims=True)
    return values * lax.rsqrt(mean_square + EPS) * gain_row


def round_up(value, step):
    return -(-value // step) * step


def mixer_kernel(
    expert_total, chunk,
    tokens_ref, mixer_gain_ref, write_ref, decay_ref, rate_ref, bias_ref,
    head_gain_ref, routes_ref, route_weights_ref,
    state_hbm, query_hbm, key_hbm, value_hbm, out_hbm,
    next_hbm, partial_ref, wext_ref,
    state, query_w, key_w, value_w, out_w, columns, readout,
    weight_sems, in_sems, out_sems,
):
    rows, heads, dim = state.shape[0], state.shape[1], state.shape[2]
    chunks = rows // chunk
    weights = [
        pltpu.make_async_copy(src, dst, weight_sems.at[i])
        for i, (src, dst) in enumerate(
            ((key_hbm, key_w), (query_hbm, query_w), (value_hbm, value_w), (out_hbm, out_w))
        )
    ]
    loads = [
        pltpu.make_async_copy(
            state_hbm.at[pl.ds(i * chunk, chunk)], state.at[pl.ds(i * chunk, chunk)], in_sems.at[i]
        )
        for i in range(chunks)
    ]
    stores = [
        pltpu.make_async_copy(
            state.at[pl.ds(i * chunk, chunk)], next_hbm.at[pl.ds(i * chunk, chunk)], out_sems.at[i]
        )
        for i in range(chunks)
    ]
    for copy in weights[:3] + loads + weights[3:]:
        copy.start()

    raw = route_weights_ref[...]
    norm = raw / jnp.sum(raw, axis=1, keepdims=True) * ROUTED_SCALE
    routes = routes_ref[...]
    lane = lax.broadcasted_iota(jnp.int32, (rows, wext_ref.shape[1]), 1)
    high = jnp.zeros(lane.shape, F32)
    for k in range(routes.shape[1]):
        hit = (lane == routes[:, k : k + 1]) | (lane == routes[:, k : k + 1] + expert_total)
        high = high + jnp.where(hit, norm[:, k : k + 1], 0.0)
    rounded = high.astype(BF16)
    low = (high - rounded.astype(F32)).astype(BF16)
    wext_ref[...] = jnp.where(lane < expert_total, rounded.astype(F32), low.astype(F32)).astype(BF16)

    normed = rms_rows(tokens_ref[...].astype(F32), mixer_gain_ref[...]).astype(BF16)
    write_rate = jax.nn.sigmoid(jnp.dot(normed, write_ref[...], preferred_element_type=F32))
    pre = jnp.dot(normed, decay_ref[...], preferred_element_type=F32) + bias_ref[...]
    softplus = jnp.maximum(pre, 0.0) + jnp.log1p(jnp.exp(-jnp.abs(pre)))
    keep = jnp.exp(-rate_ref[...] * softplus)

    def project(copy, ref):
        copy.wait()
        return jnp.dot(normed, ref[...], preferred_element_type=F32).astype(BF16).astype(F32)

    key_raw = project(weights[0], key_w)
    query_raw = project(weights[1], query_w)
    value_raw = project(weights[2], value_w)
    stride = round_up(rows, 8)
    per_head = []
    for h in range(heads):
        part = slice(h * dim, (h + 1) * dim)
        k_h, q_h = key_raw[:, part], query_raw[:, part]
        k_h = k_h * lax.rsqrt(jnp.sum(k_h * k_h, axis=-1, keepdims=True) + EPS)
        q_h = q_h * lax.rsqrt(jnp.sum(q_h * q_h, axis=-1, keepdims=True) + EPS) * dim ** (-0.5)
        columns[2 * h * stride : 2 * h * stride + rows, :] = k_h
        columns[(2 * h + 1) * stride : (2 * h + 1) * stride + rows, :] = q_h
        dots = jnp.sum(k_h * q_h, axis=-1, keepdims=True)
        per_head.append(
            (
                value_raw[:, part],
                jnp.broadcast_to(keep[:, h : h + 1], (rows, dim)),
                jnp.broadcast_to(write_rate[:, h : h + 1], (rows, dim)),
                jnp.broadcast_to(dots, (rows, dim)),
            )
        )
    turned = columns[...].T

    for i in range(chunks):
        loads[i].wait()
        for r in range(i * chunk, (i + 1) * chunk):
            for h in range(heads):
                v_h, keep_h, write_h, dots_h = (x[r : r + 1, :] for x in per_head[h])
                at = 2 * h * stride + r
                k_col = jnp.broadcast_to(turned[:, at : at + 1], (dim, dim))
                q_col = jnp.broadcast_to(turned[:, at + stride : at + stride + 1], (dim, dim))
                old = state[r, h]
                seen = jnp.sum(old * k_col, axis=0, keepdims=True)
                asked = jnp.sum(old * q_col, axis=0, keepdims=True)
                step = write_h * (v_h - keep_h * seen)
                state[r, h] = keep_h * old + k_col * step
                readout[r : r + 1, h * dim : (h + 1) * dim] = keep_h * asked + dots_h * step
        stores[i].start()

    weights[3].wait()
    total = jnp.zeros(partial_ref.shape, F32)
    for h in range(heads):
        part = slice(h * dim, (h + 1) * dim)
        head_out = rms_rows(readout[:, part], head_gain_ref[...]).astype(BF16)
        total = total + jnp.dot(head_out, out_w[part, :], preferred_element_type=F32)
    partial_ref[...] = total.astype(BF16)
    for copy in stores:
        copy.wait()


def flip(index, mask):
    bit = 1
    while bit <= mask:
        if mask & bit:
            index = index + bit - 2 * bit * ((index // bit) % 2)
        bit *= 2
    return index


def experts_kernel(
    zs, ys, tps, pad,
    tokens_ref, partial_ref, wext_ref, channel_gain_ref,
    gate_hbm, up_hbm, down_hbm, sgate_hbm, sup_hbm, sdown_hbm,
    out_ref,
    gate_w, up_w, down_w, sgate_w, sup_w, sdown_w,
    mixed, blocks, packed, near, core_send, core_recv, y_send, y_recv,
    z_send, z_recv, own_share,
    weight_sems, x_send_sems, x_recv_sems,
    agz_send_sems, agz_recv_sems, agy_send_sems, agy_recv_sems,
    agc_send_sems, agc_recv_sems,
    rsc_send_sems, rsc_recv_sems, rsy_send_sems, rsy_recv_sems,
    rsz_send_sems, rsz_recv_sems,
):
    rows, width = tokens_ref.shape
    share = width // tps
    me, tp = lax.axis_index("ep"), lax.axis_index("tp")
    core, chip = me % 2, me // 2
    y, z = chip % ys, chip // ys
    expert_total = 2 * ys * zs

    def ep_of(dz, dy, dc):
        return (flip(z, dz) * ys + flip(y, dy)) * 2 + flip(core, dc)

    weights = [
        pltpu.make_async_copy(src, dst, weight_sems.at[i])
        for i, (src, dst) in enumerate(
            (
                (sgate_hbm, sgate_w), (sup_hbm, sup_w), (sdown_hbm, sdown_w),
                (gate_hbm, gate_w), (up_hbm, up_w), (down_hbm, down_w),
            )
        )
    ]
    for copy in weights:
        copy.start()

    peers = [(ep_of(dz, 0, 0), flip(tp, dt)) for dz in range(zs) for dt in range(tps) if dz or dt]
    peers += [(ep_of(0, dy, 0), tp) for dy in range(1, ys)] + [(ep_of(0, 0, 1), tp)]
    barrier = pltpu.get_barrier_semaphore()
    for peer in peers:
        pl.semaphore_signal(barrier, inc=1, device_id=peer, device_id_type=MESH)
    pl.semaphore_wait(barrier, len(peers))

    def remote(src, dst, send_sem, recv_sem, peer):
        copy = pltpu.make_async_remote_copy(
            src_ref=src, dst_ref=dst, send_sem=send_sem, recv_sem=recv_sem,
            device_id=peer, device_id_type=MESH,
        )
        copy.start()
        return copy

    sent = []

    x_copies = [
        remote(partial_ref, mixed.at[dt - 1], x_send_sems.at[dt - 1], x_recv_sems.at[dt - 1],
               (me, flip(tp, dt)))
        for dt in range(1, tps)
    ]
    mixer_out = partial_ref[...].astype(F32)
    for dt in range(1, tps):
        x_copies[dt - 1].wait_recv()
        mixer_out = mixer_out + mixed[dt - 1].astype(F32)
    sent += x_copies
    mixer_out = mixer_out.astype(BF16).astype(F32)
    residual = (tokens_ref[...].astype(F32) + mixer_out).astype(BF16)
    expert_input = rms_rows(residual.astype(F32), channel_gain_ref[...]).astype(BF16)
    for t in range(tps):
        own_share[t] = residual[:, t * share : (t + 1) * share].astype(F32)
    blocks[0, :, :width] = expert_input
    blocks[0, :, width:] = wext_ref[...]

    def slot(dz, dy, dc):
        return (dc * zs + dz) * ys + dy

    z_copies = {
        dz: remote(blocks.at[slot(0, 0, 0)], blocks.at[slot(dz, 0, 0)],
                   agz_send_sems.at[dz], agz_recv_sems.at[dz], (ep_of(dz, 0, 0), tp))
        for dz in range(1, zs)
    }
    y_copies, c_copies = {}, {}

    def to_core(dz, dy):
        at = dz * ys + dy
        c_copies[dz, dy] = remote(
            blocks.at[slot(dz, dy, 0)], blocks.at[slot(dz, dy, 1)],
            agc_send_sems.at[at], agc_recv_sems.at[at], (ep_of(0, 0, 1), tp))

    def pack(dz, dy, dc):
        at = slot(dz, dy, dc)
        packed[at * pad : at * pad + rows, :] = blocks[at]

    def pass_on(dz):
        for dy in range(1, ys):
            at = dz * ys + dy
            y_copies[dz, dy] = remote(
                blocks.at[slot(dz, 0, 0)], blocks.at[slot(dz, dy, 0)],
                agy_send_sems.at[at], agy_recv_sems.at[at], (ep_of(0, dy, 0), tp))
        to_core(dz, 0)

    pass_on(0)

    for copy in weights[:3]:
        copy.wait()

    def gated(x, g_ref, u_ref):
        g = jnp.dot(x, g_ref[...], preferred_element_type=F32)
        u = jnp.dot(x, u_ref[...], preferred_element_type=F32)
        return (g * jax.nn.sigmoid(g) * u).astype(BF16)

    shared_act = gated(expert_input, sgate_w, sup_w)
    shared_part = jnp.dot(shared_act, sdown_w[...], preferred_element_type=F32)
    pack(0, 0, 0)
    for copy in weights[3:]:
        copy.wait()

    for dz in range(1, zs):
        z_copies[dz].wait_recv()
        pass_on(dz)
        pack(dz, 0, 0)
    for dz in range(zs):
        for dy in range(1, ys):
            y_copies[dz, dy].wait_recv()
            to_core(dz, dy)
            pack(dz, dy, 0)

    half = zs * ys * pad
    split = max(1, half // 512)

    def expert(first, count):
        x = packed[first : first + count, :width]
        act = gated(x, gate_w, up_w)
        down = jnp.dot(act, down_w[...], preferred_element_type=F32)
        spread = packed[first : first + count, width:].astype(F32)
        lane = lax.broadcasted_iota(jnp.int32, spread.shape, 1)
        mine = (lane == me) | (lane == me + expert_total)
        return down * jnp.sum(jnp.where(mine, spread, 0.0), axis=1, keepdims=True)

    piece = half // split
    per_piece = zs * ys // split
    for s in range(split):
        near[s * piece : (s + 1) * piece, :] = expert(s * piece, piece)

    for s in range(split):
        for n in range(s * per_piece, (s + 1) * per_piece):
            c_copies[n // ys, n % ys].wait_recv()
            pack(n // ys, n % ys, 1)
        far = expert(half + s * piece, piece)
        for n in range(per_piece):
            core_send[s * per_piece + n] = far[n * pad : n * pad + rows, :].astype(BF16)
        for n in range(s * per_piece, (s + 1) * per_piece):
            sent.append(remote(core_send.at[n], core_recv.at[n], rsc_send_sems.at[n],
                               rsc_recv_sems.at[n], (ep_of(0, 0, 1), tp)))
    c_returns = sent[-zs * ys:]

    def both_cores(dz, dy):
        n = dz * ys + dy
        c_returns[n].wait_recv()
        return near[n * pad : n * pad + rows, :] + core_recv[n].astype(F32)

    order = [dz for dz in range(zs - 1, -1, -1)]
    y_returns = {}
    for dz in order:
        for dy in range(1, ys):
            n = dz * ys + dy
            y_send[n] = both_cores(dz, dy).astype(BF16)
            y_returns[dz, dy] = remote(y_send.at[n], y_recv.at[n], rsy_send_sems.at[n],
                                       rsy_recv_sems.at[n], (ep_of(0, dy, 0), tp))
    z_returns = []
    for dz in order:
        total = both_cores(dz, 0)
        for dy in range(1, ys):
            y_returns[dz, dy].wait_recv()
            total = total + y_recv[dz * ys + dy].astype(F32)
        if dz == 0:
            total = total + shared_part
            for t in range(tps):
                own_share[t] = own_share[t] + total[:, t * share : (t + 1) * share]
        for t in range(tps):
            z_send[dz * tps + t] = total[:, t * share : (t + 1) * share].astype(BF16)
        for dt in range(tps):
            if dz or dt:
                at = dz * tps + dt
                z_returns.append((at, remote(
                    z_send.at[dz * tps + flip(tp, dt)], z_recv.at[at],
                    rsz_send_sems.at[at], rsz_recv_sems.at[at],
                    (ep_of(dz, 0, 0), flip(tp, dt)))))
    result = own_share[tp]
    for at, copy in reversed(z_returns):
        copy.wait_recv()
        result = result + z_recv[at].astype(F32)
    out_ref[...] = result.astype(BF16)

    sent += list(z_copies.values()) + list(y_copies.values()) + list(c_copies.values())
    sent += list(y_returns.values()) + [copy for _, copy in z_returns]
    for copy in sent:
        copy.wait_send()


def per_device(
    ep_count, tp_count,
    tokens, delta_state, mixer_gain, query_weight, key_weight, value_weight,
    write_weight, decay_weight, decay_rate, decay_bias, head_gain, out_weight,
    channel_gain, routes, route_weights, expert_gate, expert_up, expert_down,
    shared_gate, shared_up, shared_down,
):
    rows, width = tokens.shape
    heads, dim = delta_state.shape[1], delta_state.shape[2]
    hidden = expert_gate.shape[2]
    shidden = shared_gate.shape[1]
    chips = ep_count // 2
    ys = 1
    while 4 * ys * ys <= chips:
        ys *= 2
    zs = chips // ys
    extra = round_up(2 * ep_count, 128)
    share = width // tp_count
    vmem = pl.BlockSpec(memory_space=pltpu.VMEM)
    anyspace = pl.BlockSpec(memory_space=pl.ANY)
    dma = pltpu.SemaphoreType.DMA
    chunk = next(c for c in (3, 2, 1) if rows % c == 0)
    column_rows = round_up(2 * heads * round_up(rows, 8), 128)

    next_state, partial, wext = pl.pallas_call(
        functools.partial(mixer_kernel, ep_count, chunk),
        out_shape=(
            jax.ShapeDtypeStruct(delta_state.shape, F32),
            jax.ShapeDtypeStruct((rows, width), BF16),
            jax.ShapeDtypeStruct((rows, extra), BF16),
        ),
        in_specs=[vmem] * 9 + [anyspace] * 5,
        out_specs=(anyspace, vmem, vmem),
        scratch_shapes=[
            pltpu.VMEM(delta_state.shape, F32),
            pltpu.VMEM(query_weight.shape, BF16),
            pltpu.VMEM(key_weight.shape, BF16),
            pltpu.VMEM(value_weight.shape, BF16),
            pltpu.VMEM(out_weight.shape, BF16),
            pltpu.VMEM((column_rows, dim), F32),
            pltpu.VMEM((rows, heads * dim), F32),
            dma((4,)), dma((rows // chunk,)), dma((rows // chunk,)),
        ],
    )(
        tokens, mixer_gain.reshape(1, width), write_weight, decay_weight,
        decay_rate.reshape(1, heads), decay_bias.reshape(1, heads), head_gain.reshape(1, dim),
        routes, route_weights, delta_state, query_weight, key_weight, value_weight, out_weight,
    )

    pad = round_up(rows, 16)
    zy = zs * ys
    layer_out = pl.pallas_call(
        functools.partial(experts_kernel, zs, ys, tp_count, pad),
        out_shape=jax.ShapeDtypeStruct((rows, share), BF16),
        in_specs=[vmem] * 4 + [anyspace] * 6,
        out_specs=vmem,
        scratch_shapes=[
            pltpu.VMEM((width, hidden), BF16), pltpu.VMEM((width, hidden), BF16),
            pltpu.VMEM((hidden, width), BF16),
            pltpu.VMEM((width, shidden), BF16), pltpu.VMEM((width, shidden), BF16),
            pltpu.VMEM((shidden, width), BF16),
            pltpu.VMEM((max(1, tp_count - 1), rows, width), BF16),
            pltpu.VMEM((2 * zy, rows, width + extra), BF16),
            pltpu.VMEM((2 * zy * pad, width + extra), BF16),
            pltpu.VMEM((zy * pad, width), F32),
            pltpu.VMEM((zy, rows, width), BF16), pltpu.VMEM((zy, rows, width), BF16),
            pltpu.VMEM((zy, rows, width), BF16), pltpu.VMEM((zy, rows, width), BF16),
            pltpu.VMEM((zs * tp_count, rows, share), BF16),
            pltpu.VMEM((zs * tp_count, rows, share), BF16),
            pltpu.VMEM((tp_count, rows, share), F32),
            dma((6,)), dma((tp_count,)), dma((tp_count,)),
            dma((zs,)), dma((zs,)), dma((zy,)), dma((zy,)), dma((zy,)), dma((zy,)),
            dma((zy,)), dma((zy,)), dma((zy,)), dma((zy,)),
            dma((zs * tp_count,)), dma((zs * tp_count,)),
        ],
        compiler_params=pltpu.CompilerParams(collective_id=0, has_side_effects=True),
    )(
        tokens, partial, wext, channel_gain.reshape(1, width),
        expert_gate.reshape(width, hidden), expert_up.reshape(width, hidden),
        expert_down.reshape(hidden, width), shared_gate, shared_up, shared_down,
    )
    return layer_out, next_state


def solution(mesh):
    return jax.shard_map(
        functools.partial(per_device, mesh.shape["ep"], mesh.shape["tp"]),
        mesh=mesh,
        in_specs=(
            P("ep", None),
            P("ep", "tp", None, None),
            P(),
            P(None, "tp"),
            P(None, "tp"),
            P(None, "tp"),
            P(None, "tp"),
            P(None, "tp"),
            P("tp"),
            P("tp"),
            P(),
            P("tp", None),
            P(),
            P("ep", None),
            P("ep", None),
            P("ep", None, "tp"),
            P("ep", None, "tp"),
            P("ep", "tp", None),
            P(None, "tp"),
            P(None, "tp"),
            P("tp", None),
        ),
        out_specs=(P("ep", "tp"), P("ep", "tp", None, None)),
        check_vma=False,
    )
```

```python
import functools

import jax
import jax.numpy as jnp
from jax import lax
from jax.experimental import pallas as pl
from jax.experimental.pallas import tpu as pltpu
from jax.sharding import PartitionSpec as P

EPS = 1e-06
ROUTED_SCALE = 2.5
MESH = pl.DeviceIdType.MESH
F32 = jnp.float32
BF16 = jnp.bfloat16


def rms_rows(values, gain_row):
    mean_square = jnp.mean(values * values, axis=-1, keepdims=True)
    return values * lax.rsqrt(mean_square + EPS) * gain_row


def round_up(value, step):
    return -(-value // step) * step


def mixer_kernel(
    expert_total, chunk,
    tokens_ref, mixer_gain_ref, write_ref, decay_ref, rate_ref, bias_ref,
    head_gain_ref, routes_ref, route_weights_ref,
    state_hbm, query_hbm, key_hbm, value_hbm, out_hbm,
    next_hbm, partial_ref, wext_ref,
    state, query_w, key_w, value_w, out_w, columns, readout, spread,
    weight_sems, in_sems, out_sems,
):
    rows, heads, dim = state.shape[0], state.shape[1], state.shape[2]
    chunks = rows // chunk
    weights = [
        pltpu.make_async_copy(src, dst, weight_sems.at[i])
        for i, (src, dst) in enumerate(
            ((key_hbm, key_w), (query_hbm, query_w), (value_hbm, value_w), (out_hbm, out_w))
        )
    ]
    loads = [
        pltpu.make_async_copy(
            state_hbm.at[pl.ds(i * chunk, chunk)], state.at[pl.ds(i * chunk, chunk)], in_sems.at[i]
        )
        for i in range(chunks)
    ]
    stores = [
        pltpu.make_async_copy(
            state.at[pl.ds(i * chunk, chunk)], next_hbm.at[pl.ds(i * chunk, chunk)], out_sems.at[i]
        )
        for i in range(chunks)
    ]
    for copy in weights[:3] + loads + weights[3:]:
        copy.start()

    raw = route_weights_ref[...]
    norm = raw / jnp.sum(raw, axis=0, keepdims=True) * ROUTED_SCALE
    routes = routes_ref[...]
    row = lax.broadcasted_iota(jnp.int32, (spread.shape[0], rows), 0)
    high = jnp.zeros(row.shape, F32)
    for k in range(routes.shape[0]):
        named = routes[k : k + 1, :]
        hit = (row == named) | (row == named + expert_total)
        high = high + jnp.where(hit, norm[k : k + 1, :], 0.0)
    rounded = high.astype(BF16).astype(F32)
    spread[:, :rows] = jnp.where(row < expert_total, rounded, high - rounded)
    wext_ref[...] = spread[...].T[:rows, :].astype(BF16)

    normed = rms_rows(tokens_ref[...].astype(F32), mixer_gain_ref[...]).astype(BF16)
    wide = normed.astype(F32)

    def per_head_dot(ref):
        table = ref[...].astype(F32)
        return [jnp.sum(wide * table[h : h + 1, :], axis=-1, keepdims=True) for h in range(heads)]

    write_rate = [jax.nn.sigmoid(x) for x in per_head_dot(write_ref)]
    keep = []
    for h, pre in enumerate(per_head_dot(decay_ref)):
        pre = pre + bias_ref[:, h : h + 1]
        softplus = jnp.maximum(pre, 0.0) + jnp.log1p(jnp.exp(-jnp.abs(pre)))
        keep.append(jnp.exp(-rate_ref[:, h : h + 1] * softplus))

    def project(copy, ref):
        copy.wait()
        return jnp.dot(normed, ref[...], preferred_element_type=F32).astype(BF16).astype(F32)

    key_raw = project(weights[0], key_w)
    query_raw = project(weights[1], query_w)
    value_raw = project(weights[2], value_w)
    stride = round_up(rows, 8)
    per_head = []
    for h in range(heads):
        part = slice(h * dim, (h + 1) * dim)
        k_h, q_h = key_raw[:, part], query_raw[:, part]
        k_h = k_h * lax.rsqrt(jnp.sum(k_h * k_h, axis=-1, keepdims=True) + EPS)
        q_h = q_h * lax.rsqrt(jnp.sum(q_h * q_h, axis=-1, keepdims=True) + EPS) * dim ** (-0.5)
        columns[2 * h * stride : 2 * h * stride + rows, :] = k_h
        columns[(2 * h + 1) * stride : (2 * h + 1) * stride + rows, :] = q_h
        dots = jnp.sum(k_h * q_h, axis=-1, keepdims=True)
        per_head.append(
            (
                value_raw[:, part],
                jnp.broadcast_to(keep[h], (rows, dim)),
                jnp.broadcast_to(write_rate[h], (rows, dim)),
                jnp.broadcast_to(dots, (rows, dim)),
            )
        )
    turned = columns[...].T

    for i in range(chunks):
        loads[i].wait()
        for r in range(i * chunk, (i + 1) * chunk):
            for h in range(heads):
                v_h, keep_h, write_h, dots_h = (x[r : r + 1, :] for x in per_head[h])
                at = 2 * h * stride + r
                k_col = jnp.broadcast_to(turned[:, at : at + 1], (dim, dim))
                q_col = jnp.broadcast_to(turned[:, at + stride : at + stride + 1], (dim, dim))
                old = state[r, h]
                seen = jnp.sum(old * k_col, axis=0, keepdims=True)
                asked = jnp.sum(old * q_col, axis=0, keepdims=True)
                step = write_h * (v_h - keep_h * seen)
                state[r, h] = keep_h * old + k_col * step
                readout[r : r + 1, h * dim : (h + 1) * dim] = keep_h * asked + dots_h * step
        stores[i].start()

    weights[3].wait()
    total = jnp.zeros(partial_ref.shape, F32)
    for h in range(heads):
        part = slice(h * dim, (h + 1) * dim)
        head_out = rms_rows(readout[:, part], head_gain_ref[...]).astype(BF16)
        total = total + jnp.dot(head_out, out_w[part, :], preferred_element_type=F32)
    partial_ref[...] = total.astype(BF16)
    for copy in stores:
        copy.wait()


def flip(index, mask):
    bit = 1
    while bit <= mask:
        if mask & bit:
            index = index + bit - 2 * bit * ((index // bit) % 2)
        bit *= 2
    return index


def experts_kernel(
    zs, ys, tps, pad,
    tokens_ref, partial_ref, wext_ref, channel_gain_ref,
    gate_hbm, up_hbm, down_hbm, sgate_hbm, sup_hbm, sdown_hbm,
    out_ref,
    gate_w, up_w, down_w, sgate_w, sup_w, sdown_w,
    mixed, blocks, packed, near, core_send, core_recv, y_send, y_recv,
    z_send, z_recv, own_share,
    weight_sems, x_send_sems, x_recv_sems,
    agz_send_sems, agz_recv_sems, agy_send_sems, agy_recv_sems,
    agc_send_sems, agc_recv_sems,
    rsc_send_sems, rsc_recv_sems, rsy_send_sems, rsy_recv_sems,
    rsz_send_sems, rsz_recv_sems,
):
    rows, width = tokens_ref.shape
    share = width // tps
    me, tp = lax.axis_index("ep"), lax.axis_index("tp")
    core, chip = me % 2, me // 2
    y, z = chip % ys, chip // ys
    expert_total = 2 * ys * zs

    def ep_of(dz, dy, dc):
        return (flip(z, dz) * ys + flip(y, dy)) * 2 + flip(core, dc)

    weights = [
        pltpu.make_async_copy(src, dst, weight_sems.at[i])
        for i, (src, dst) in enumerate(
            (
                (sgate_hbm, sgate_w), (sup_hbm, sup_w), (sdown_hbm, sdown_w),
                (gate_hbm, gate_w), (up_hbm, up_w), (down_hbm, down_w),
            )
        )
    ]
    for copy in weights:
        copy.start()

    peers = [(ep_of(dz, 0, 0), flip(tp, dt)) for dz in range(zs) for dt in range(tps) if dz or dt]
    peers += [(ep_of(0, dy, 0), tp) for dy in range(1, ys)] + [(ep_of(0, 0, 1), tp)]
    barrier = pltpu.get_barrier_semaphore()
    for peer in peers:
        pl.semaphore_signal(barrier, inc=1, device_id=peer, device_id_type=MESH)
    pl.semaphore_wait(barrier, len(peers))

    def remote(src, dst, send_sem, recv_sem, peer):
        copy = pltpu.make_async_remote_copy(
            src_ref=src, dst_ref=dst, send_sem=send_sem, recv_sem=recv_sem,
            device_id=peer, device_id_type=MESH,
        )
        copy.start()
        return copy

    sent = []

    x_copies = [
        remote(partial_ref, mixed.at[dt - 1], x_send_sems.at[dt - 1], x_recv_sems.at[dt - 1],
               (me, flip(tp, dt)))
        for dt in range(1, tps)
    ]
    mixer_out = partial_ref[...].astype(F32)
    for dt in range(1, tps):
        x_copies[dt - 1].wait_recv()
        mixer_out = mixer_out + mixed[dt - 1].astype(F32)
    sent += x_copies
    mixer_out = mixer_out.astype(BF16).astype(F32)
    residual = (tokens_ref[...].astype(F32) + mixer_out).astype(BF16)
    expert_input = rms_rows(residual.astype(F32), channel_gain_ref[...]).astype(BF16)
    for t in range(tps):
        own_share[t] = residual[:, t * share : (t + 1) * share].astype(F32)
    blocks[0, :, :width] = expert_input
    blocks[0, :, width:] = wext_ref[...]

    def slot(dz, dy, dc):
        return (dz * 2 + dc) * ys + dy

    order = [0] + list(range(zs - 1, 0, -1))
    z_copies = {
        dz: remote(blocks.at[slot(0, 0, 0)], blocks.at[slot(dz, 0, 0)],
                   agz_send_sems.at[dz], agz_recv_sems.at[dz], (ep_of(dz, 0, 0), tp))
        for dz in order[1:]
    }
    y_copies, c_copies = {}, {}

    def to_core(dz, dy):
        at = dz * ys + dy
        c_copies[dz, dy] = remote(
            blocks.at[slot(dz, dy, 0)], blocks.at[slot(dz, dy, 1)],
            agc_send_sems.at[at], agc_recv_sems.at[at], (ep_of(0, 0, 1), tp))

    def pack(dz, dy, dc):
        at = slot(dz, dy, dc)
        packed[at * pad : at * pad + rows, :] = blocks[at]

    def pass_on(dz):
        for dy in range(1, ys):
            at = dz * ys + dy
            y_copies[dz, dy] = remote(
                blocks.at[slot(dz, 0, 0)], blocks.at[slot(dz, dy, 0)],
                agy_send_sems.at[at], agy_recv_sems.at[at], (ep_of(0, dy, 0), tp))
        to_core(dz, 0)

    pass_on(0)

    for copy in weights[:3]:
        copy.wait()

    def gated(x, g_ref, u_ref):
        g = jnp.dot(x, g_ref[...], preferred_element_type=F32)
        u = jnp.dot(x, u_ref[...], preferred_element_type=F32)
        return (g * jax.nn.sigmoid(g) * u).astype(BF16)

    shared_act = gated(expert_input, sgate_w, sup_w)
    shared_part = jnp.dot(shared_act, sdown_w[...], preferred_element_type=F32)
    for copy in weights[3:]:
        copy.wait()

    def gather_z(dz):
        if dz:
            z_copies[dz].wait_recv()
            pass_on(dz)
        pack(dz, 0, 0)

    def gather_y(dz):
        for dy in range(1, ys):
            y_copies[dz, dy].wait_recv()
            to_core(dz, dy)
            pack(dz, dy, 0)

    half = ys * pad
    c_returns, y_returns, z_returns = {}, {}, []

    def run_expert(dz):
        for dy in range(ys):
            c_copies[dz, dy].wait_recv()
            pack(dz, dy, 1)
        first = slot(dz, 0, 0) * pad
        x = packed[first : first + 2 * half, :width]
        act = gated(x, gate_w, up_w)
        down = jnp.dot(act, down_w[...], preferred_element_type=F32)
        spread = packed[first : first + 2 * half, width:].astype(F32)
        lane = lax.broadcasted_iota(jnp.int32, spread.shape, 1)
        mine = (lane == me) | (lane == me + expert_total)
        down = down * jnp.sum(jnp.where(mine, spread, 0.0), axis=1, keepdims=True)
        for dy in range(ys - 1, -1, -1):
            n = dz * ys + dy
            core_send[n] = down[half + dy * pad : half + dy * pad + rows, :].astype(BF16)
            c_returns[n] = remote(core_send.at[n], core_recv.at[n], rsc_send_sems.at[n],
                                  rsc_recv_sems.at[n], (ep_of(0, 0, 1), tp))
        near[dz * half : (dz + 1) * half, :] = down[:half, :]

    def both_cores(dz, dy):
        n = dz * ys + dy
        c_returns[n].wait_recv()
        return near[n * pad : n * pad + rows, :] + core_recv[n].astype(F32)

    def return_y(dz):
        for dy in range(1, ys):
            n = dz * ys + dy
            y_send[n] = both_cores(dz, dy).astype(BF16)
            y_returns[n] = remote(y_send.at[n], y_recv.at[n], rsy_send_sems.at[n],
                                  rsy_recv_sems.at[n], (ep_of(0, dy, 0), tp))

    def return_z(dz):
        total = both_cores(dz, 0)
        for dy in range(1, ys):
            y_returns[dz * ys + dy].wait_recv()
            total = total + y_recv[dz * ys + dy].astype(F32)
        if dz == 0:
            total = total + shared_part
            for t in range(tps):
                own_share[t] = own_share[t] + total[:, t * share : (t + 1) * share]
        for t in range(tps):
            z_send[dz * tps + t] = total[:, t * share : (t + 1) * share].astype(BF16)
        for dt in range(tps - 1, -1, -1):
            if dz or dt:
                at = dz * tps + dt
                z_returns.append((at, remote(
                    z_send.at[dz * tps + flip(tp, dt)], z_recv.at[at],
                    rsz_send_sems.at[at], rsz_recv_sems.at[at],
                    (ep_of(dz, 0, 0), flip(tp, dt)))))

    stages = (gather_z, gather_y, run_expert, return_y, return_z)
    for step in range(zs + len(stages) - 1):
        for lag, stage in enumerate(stages):
            if 0 <= step - lag < zs:
                stage(order[step - lag])
    result = own_share[tp]
    for at, copy in z_returns:
        copy.wait_recv()
        result = result + z_recv[at].astype(F32)
    out_ref[...] = result.astype(BF16)

    sent += list(z_copies.values()) + list(y_copies.values()) + list(c_copies.values())
    sent += list(c_returns.values()) + list(y_returns.values()) + [copy for _, copy in z_returns]
    for copy in sent:
        copy.wait_send()


def per_device(
    ep_count, tp_count,
    tokens, delta_state, mixer_gain, query_weight, key_weight, value_weight,
    write_weight, decay_weight, decay_rate, decay_bias, head_gain, out_weight,
    channel_gain, routes, route_weights, expert_gate, expert_up, expert_down,
    shared_gate, shared_up, shared_down,
):
    rows, width = tokens.shape
    heads, dim = delta_state.shape[1], delta_state.shape[2]
    hidden = expert_gate.shape[2]
    shidden = shared_gate.shape[1]
    chips = ep_count // 2
    ys = 1
    while 4 * ys * ys <= chips:
        ys *= 2
    zs = chips // ys
    extra = round_up(2 * ep_count, 128)
    share = width // tp_count
    vmem = pl.BlockSpec(memory_space=pltpu.VMEM)
    anyspace = pl.BlockSpec(memory_space=pl.ANY)
    dma = pltpu.SemaphoreType.DMA
    chunk = next(c for c in (3, 2, 1) if rows % c == 0)
    column_rows = round_up(2 * heads * round_up(rows, 8), 128)

    next_state, partial, wext = pl.pallas_call(
        functools.partial(mixer_kernel, ep_count, chunk),
        out_shape=(
            jax.ShapeDtypeStruct(delta_state.shape, F32),
            jax.ShapeDtypeStruct((rows, width), BF16),
            jax.ShapeDtypeStruct((rows, extra), BF16),
        ),
        in_specs=[vmem] * 9 + [anyspace] * 5,
        out_specs=(anyspace, vmem, vmem),
        scratch_shapes=[
            pltpu.VMEM(delta_state.shape, F32),
            pltpu.VMEM(query_weight.shape, BF16),
            pltpu.VMEM(key_weight.shape, BF16),
            pltpu.VMEM(value_weight.shape, BF16),
            pltpu.VMEM(out_weight.shape, BF16),
            pltpu.VMEM((column_rows, dim), F32),
            pltpu.VMEM((rows, heads * dim), F32),
            pltpu.VMEM((extra, round_up(rows, 128)), F32),
            dma((4,)), dma((rows // chunk,)), dma((rows // chunk,)),
        ],
    )(
        tokens, mixer_gain.reshape(1, width), write_weight.T, decay_weight.T,
        decay_rate.reshape(1, heads), decay_bias.reshape(1, heads), head_gain.reshape(1, dim),
        routes.T, route_weights.T, delta_state, query_weight, key_weight, value_weight, out_weight,
    )

    pad = round_up(rows, 16)
    zy = zs * ys
    layer_out = pl.pallas_call(
        functools.partial(experts_kernel, zs, ys, tp_count, pad),
        out_shape=jax.ShapeDtypeStruct((rows, share), BF16),
        in_specs=[vmem] * 4 + [anyspace] * 6,
        out_specs=vmem,
        scratch_shapes=[
            pltpu.VMEM((width, hidden), BF16), pltpu.VMEM((width, hidden), BF16),
            pltpu.VMEM((hidden, width), BF16),
            pltpu.VMEM((width, shidden), BF16), pltpu.VMEM((width, shidden), BF16),
            pltpu.VMEM((shidden, width), BF16),
            pltpu.VMEM((max(1, tp_count - 1), rows, width), BF16),
            pltpu.VMEM((2 * zy, rows, width + extra), BF16),
            pltpu.VMEM((2 * zy * pad, width + extra), BF16),
            pltpu.VMEM((zy * pad, width), F32),
            pltpu.VMEM((zy, rows, width), BF16), pltpu.VMEM((zy, rows, width), BF16),
            pltpu.VMEM((zy, rows, width), BF16), pltpu.VMEM((zy, rows, width), BF16),
            pltpu.VMEM((zs * tp_count, rows, share), BF16),
            pltpu.VMEM((zs * tp_count, rows, share), BF16),
            pltpu.VMEM((tp_count, rows, share), F32),
            dma((6,)), dma((tp_count,)), dma((tp_count,)),
            dma((zs,)), dma((zs,)), dma((zy,)), dma((zy,)), dma((zy,)), dma((zy,)),
            dma((zy,)), dma((zy,)), dma((zy,)), dma((zy,)),
            dma((zs * tp_count,)), dma((zs * tp_count,)),
        ],
        compiler_params=pltpu.CompilerParams(collective_id=0, has_side_effects=True),
    )(
        tokens, partial, wext, channel_gain.reshape(1, width),
        expert_gate.reshape(width, hidden), expert_up.reshape(width, hidden),
        expert_down.reshape(hidden, width), shared_gate, shared_up, shared_down,
    )
    return layer_out, next_state


def solution(mesh):
    return jax.shard_map(
        functools.partial(per_device, mesh.shape["ep"], mesh.shape["tp"]),
        mesh=mesh,
        in_specs=(
            P("ep", None),
            P("ep", "tp", None, None),
            P(),
            P(None, "tp"),
            P(None, "tp"),
            P(None, "tp"),
            P(None, "tp"),
            P(None, "tp"),
            P("tp"),
            P("tp"),
            P(),
            P("tp", None),
            P(),
            P("ep", None),
            P("ep", None),
            P("ep", None, "tp"),
            P("ep", None, "tp"),
            P("ep", "tp", None),
            P(None, "tp"),
            P(None, "tp"),
            P("tp", None),
        ),
        out_specs=(P("ep", "tp"), P("ep", "tp", None, None)),
        check_vma=False,
    )
```
